256 devices in a mesh: sp: 64 (over z, y, core), tp: 4 (over x).
Axes of the slice: x: 4, y: 4, z: 8, core: 2. Of those that a mesh axis runs over, the one named last changes fastest.
Arguments:
- queries: bfloat16 [49152, 1536], P('sp', 'tp'), may hold values from -130 to 130, as said below
- keys: bfloat16 [49152, 512], P('sp', 'tp'), may hold values from -6 to 6
- values: bfloat16 [49152, 512], P('sp', 'tp'), may hold values from -6 to 6
- residual: bfloat16 [49152, 2048], P(('sp', 'tp')), may hold values from -6 to 6
- sinks: float32 [12], P('tp'), may hold values from 2 to 6
- out_weight: bfloat16 [1536, 2048], P('tp'), may hold values from -0.15625 to 0.15625
- up_weight: bfloat16 [2048, 8192], P('sp', 'tp'), may hold values from -0.125 to 0.125
- down_weight: bfloat16 [8192, 2048], P('tp', 'sp'), may hold values from -0.0625 to 0.0625
- gains: float32 [2, 2048], replicated, may hold values from 0.1 to 1.9
- biases: float32 [2, 2048], replicated, may hold values from -3 to 3
Outputs:
- layer_out: bfloat16 [49152, 2048], P(('sp', 'tp'))
The draws below stay inside these ranges and needn't reach their ends.
Inputs may be any that keep to these rules, and one draw needn't show every extreme that they name: `queries`: entries of order one, with some rows far larger in some draws.
All inputs are finite; a program needn't handle non-finite values.
Results may differ from the reference program's by a relative error of at most 0.0095.
Values may be sent and summed in bfloat16 or wider, within the bound.
No kernel may reach another device: no remote copies, remote signals or barrier semaphores. Data moves between devices by JAX's collectives and lax.ppermute only.
A program may use at most 128 MiB of HBM per device.

```python
import jax
import jax.numpy as jnp
from jax import lax

D = 2048
HEADS = 12
KV_HEADS = 4
HEAD = 128
FF = 8192
WINDOW = 128
TOKENS = 49152
Q_W = 1536
KV_W = 512
N_TP = 4


def base_keys(key):
    drawn = jax.random.normal(jax.random.fold_in(key, 11), (TOKENS, KV_HEADS * HEAD), jnp.float32)
    return jnp.clip(drawn, -6.0, 6.0)


def draw_keys(key, part):
    return base_keys(key).astype(jnp.bfloat16)


def draw_queries(key, part):
    drawn = jnp.clip(jax.random.normal(jax.random.fold_in(key, 12), (TOKENS, HEADS * HEAD), jnp.float32), -6.0, 6.0)
    return drawn.astype(jnp.bfloat16)


def shard_levels(own_key, extent, pieces, low, high):
    level = 1.0
    for axis_at, blocks in pieces:
        steps = jax.random.uniform(jax.random.fold_in(jax.random.fold_in(own_key, 6), axis_at), (blocks,), jnp.float32, low / len(pieces), high / len(pieces))
        level = level * jnp.repeat(jnp.exp(steps), extent[axis_at] // blocks).reshape((-1,) + (1,) * (len(extent) - 1 - axis_at))
    return level


def gaussian(stream_key, shape, scale, limit, split=(), kind=jnp.bfloat16):
    entries = jax.random.normal(stream_key, shape, jnp.float32) * scale
    if len(split) > 0:
        entries = shard_levels(stream_key, shape, split, -0.22, 0.18) * entries
    return jnp.clip(entries, min=-limit, max=limit).astype(kind)


def setup_inputs(seed: int = 0) -> dict:
    streams_of = jax.random.split(jax.random.key(seed), 11)
    return {
        "queries": draw_queries(jax.random.fold_in(streams_of[10], 71), 0),
        "keys": draw_keys(jax.random.fold_in(streams_of[10], 71), 0),
        "values": gaussian(streams_of[2], (TOKENS, KV_W), 1.0, 6.0, ((0, 64), (1, 4))),
        "residual": gaussian(streams_of[3], (TOKENS, D), 1.0, 6.0, ((0, 256),)),
        "sinks": jnp.clip(2.0 + 4.0 * jax.random.uniform(streams_of[4], (HEADS,), jnp.float32) ** shard_levels(streams_of[4], (HEADS,), ((0, 4),), -0.2, 0.2), 2.0, 6.0),
        "out_weight": gaussian(streams_of[5], (Q_W, D), Q_W ** -0.5, 0.15625, ((0, 4),)),
        "up_weight": gaussian(streams_of[6], (D, FF), D ** -0.5, 0.125, ((0, 64), (1, 4))),
        "down_weight": gaussian(streams_of[7], (FF, D), FF ** -0.5, 0.0625, ((0, 4), (1, 64))),
        "gains": jnp.clip(1.0 + 0.18 * jax.random.normal(streams_of[8], (2, D), jnp.float32), 0.1, 1.9),
        "biases": gaussian(streams_of[9], (2, D), 0.5, 3.0, (), jnp.float32),
    }


deep_alpha = 1.6817928
norm_eps = 1e-05
neg_big = -1e+30

def layer_norm(stream, gain, bias):
    mean = lax.optimization_barrier(jnp.mean(stream, axis=-1, keepdims=True))
    spread = lax.optimization_barrier(jnp.mean(jnp.square(stream - mean), axis=-1, keepdims=True))
    return ((stream - mean) * lax.rsqrt(spread + norm_eps) * gain + bias).astype(jnp.bfloat16)

def window_attention(queries, keys, values, sinks):
    total = keys.shape[0]
    blocks = total // WINDOW
    group = HEADS // KV_HEADS
    q_blocks = queries.reshape(blocks, WINDOW, KV_HEADS, group, HEAD).astype(jnp.float32)
    padding = jnp.zeros((WINDOW, KV_HEADS, HEAD), jnp.bfloat16)
    key_ext = jnp.concatenate([padding, keys.reshape(total, KV_HEADS, HEAD)], axis=0)
    val_ext = jnp.concatenate([padding, values.reshape(total, KV_HEADS, HEAD)], axis=0)
    key_win = jnp.concatenate([key_ext[:total].reshape(blocks, WINDOW, KV_HEADS, HEAD), key_ext[WINDOW:].reshape(blocks, WINDOW, KV_HEADS, HEAD)], axis=1)
    val_win = jnp.concatenate([val_ext[:total].reshape(blocks, WINDOW, KV_HEADS, HEAD), val_ext[WINDOW:].reshape(blocks, WINDOW, KV_HEADS, HEAD)], axis=1)
    logits = jnp.einsum('nqkgd,nskd->nkgqs', q_blocks, key_win.astype(jnp.float32)) * HEAD ** (-0.5)
    q_index = jnp.arange(WINDOW, dtype=jnp.int32)[:, None]
    k_index = jnp.arange(2 * WINDOW, dtype=jnp.int32)[None, :]
    dist = q_index + WINDOW - k_index
    block_id = jnp.arange(blocks, dtype=jnp.int32)[:, None, None]
    key_pos = block_id * WINDOW - WINDOW + k_index
    valid = (dist >= 0) & (dist < WINDOW) & (key_pos >= 0)
    heads = jnp.arange(HEADS, dtype=jnp.float32)
    slopes = jnp.exp2(-8.0 * (heads + 1.0) / HEADS).reshape(KV_HEADS, group)[:, :, None, None]
    logits = logits - slopes * dist.astype(jnp.float32)
    logits = jnp.where(valid[:, None, None], logits, neg_big)
    sink = sinks.reshape(KV_HEADS, group)[:, :, None, None]
    top = jnp.maximum(lax.optimization_barrier(jnp.max(logits, axis=-1, keepdims=True)), sink)
    probs = jnp.exp(logits - top)
    denom = lax.optimization_barrier(jnp.sum(probs, axis=-1, keepdims=True)) + jnp.exp(sink - top)
    weight = (probs / denom).astype(jnp.bfloat16)
    attended = jnp.einsum('nkgqs,nskd->nqkgd', weight.astype(jnp.float32), val_win.astype(jnp.float32))
    return attended.astype(jnp.bfloat16).reshape(total, Q_W)

def reference(queries, keys, values, residual, sinks, out_weight, up_weight, down_weight, gains, biases):
    attended = window_attention(queries, keys, values, sinks)
    width = Q_W // N_TP
    mix = jnp.zeros((TOKENS, D), jnp.float32)
    for group_id in range(N_TP):
        term = jnp.dot(attended[:, group_id * width:(group_id + 1) * width], out_weight[group_id * width:(group_id + 1) * width], preferred_element_type=jnp.float32).astype(jnp.bfloat16)
        mix = mix + term.astype(jnp.float32)
    normed = layer_norm(deep_alpha * residual.astype(jnp.float32) + mix, gains[0], biases[0])
    hidden = FF // N_TP
    ffn = jnp.zeros((TOKENS, D), jnp.float32)
    for group_id in range(N_TP):
        upward = jnp.dot(normed, up_weight[:, group_id * hidden:(group_id + 1) * hidden], preferred_element_type=jnp.float32)
        act = jnp.square(jax.nn.relu(upward)).astype(jnp.bfloat16)
        term = jnp.dot(act, down_weight[group_id * hidden:(group_id + 1) * hidden], preferred_element_type=jnp.float32).astype(jnp.bfloat16)
        ffn = ffn + term.astype(jnp.float32)
    return layer_norm(deep_alpha * normed.astype(jnp.float32) + ffn, gains[1], biases[1])
```

```python
import functools

import jax
import jax.numpy as jnp
from jax import lax
from jax.experimental import pallas as pl
from jax.experimental.pallas import tpu as pltpu
from jax.sharding import PartitionSpec as P

HEADS = 12
HEAD = 128
WINDOW = 128
Y, Z = 4, 8

deep_alpha = 1.6817928
norm_eps = 1e-05
neg_big = -1e30


VMEM = pl.BlockSpec(memory_space=pltpu.VMEM)
SMEM = pl.BlockSpec(memory_space=pltpu.SMEM)
HBM = pl.BlockSpec(memory_space=pltpu.HBM)


def call(body, outs, args, specs, flops, scratch=(), name=None):
    return pl.pallas_call(
        body,
        out_shape=outs,
        in_specs=specs,
        out_specs=jax.tree.map(lambda _: VMEM, outs),
        scratch_shapes=list(scratch),
        compiler_params=pltpu.CompilerParams(vmem_limit_bytes=56 * 2**20),
        cost_estimate=pl.CostEstimate(flops=flops, transcendentals=0, bytes_accessed=0),
        name=name,
    )(*args)


def sp_route(move):
    pairs = []
    for i in range(Z * Y * 2):
        z, y, c = move(i // (2 * Y), i // 2 % Y, i % 2)
        pairs.append((i, z % Z * 2 * Y + y % Y * 2 + c))
    return pairs


def z_move(block, step):
    return lax.ppermute(block, "sp", sp_route(lambda z, y, c: (z + step, y, c)))


def y_move(block, step):
    return lax.ppermute(block, "sp", sp_route(lambda z, y, c: (z, y + step, c)))


def core_swap(block):
    return lax.ppermute(block, "sp", sp_route(lambda z, y, c: (z, y, 1 - c)))


def x_move(block, step):
    count = lax.axis_size("tp")
    return lax.ppermute(block, "tp", [(i, (i + step) % count) for i in range(count)])


def from_behind(block, axis, distance):
    devices = range(lax.axis_size(axis))
    route = [(i - distance, i) for i in devices if i - distance in devices]
    return lax.ppermute(block, axis, route)


def ring(block, move, count):
    down, up = [block], [block]
    for _ in range(count // 2 - 1):
        down.append(move(down[-1], 1))
        up.append(move(up[-1], -1))
    half = block.shape[0] // 2
    far_top = move(down[-1][:half], 1)
    far_bottom = move(up[-1][half:], -1)
    return [block] + down[1:], up[1:], [far_top, far_bottom]


def attend_body(info, sinks, slopes, q, k, v, halo, w, *rest, half, rows, group):
    outs, (k_ext, v_ext) = rest[:-2], rest[-2:]
    tokens = k.shape[0]
    k_ext[:WINDOW] = halo[0]
    v_ext[:WINDOW] = halo[1]
    k_ext[WINDOW:] = k[...]
    v_ext[WINDOW:] = v[...]
    rank, offset = info[0], info[1]
    span = rows + WINDOW
    shape = (rows, span)
    q_index = lax.broadcasted_iota(jnp.int32, shape, 0)
    k_index = lax.broadcasted_iota(jnp.int32, shape, 1)
    dist = q_index + WINDOW - k_index
    in_window = (dist >= 0) & (dist < WINDOW)
    dist_f = dist.astype(jnp.float32)
    blocks = tokens // (2 * rows)
    for rel, out in enumerate(outs):
        start = (rank + rel) % blocks * (2 * rows) + half * rows
        start = pl.multiple_of(start, rows)
        key = k_ext[pl.ds(start, span), :]
        val = v_ext[pl.ds(start, span), :]
        valid = in_window & (offset + start - WINDOW + k_index >= 0)
        heads = []
        for g in range(group):
            query = q[pl.ds(start, rows), g * HEAD : (g + 1) * HEAD]
            logits = lax.dot_general(
                query, key, (((1,), (1,)), ((), ())), preferred_element_type=jnp.float32
            ) * HEAD ** (-0.5)
            logits = logits - slopes[g] * dist_f
            logits = jnp.where(valid, logits, neg_big)
            top = jnp.maximum(jnp.max(logits, axis=-1, keepdims=True), sinks[g])
            probs = jnp.exp(logits - top)
            denom = jnp.sum(probs, axis=-1, keepdims=True) + jnp.exp(sinks[g] - top)
            weight = (probs / denom).astype(jnp.bfloat16)
            heads.append(
                jnp.dot(weight, val, preferred_element_type=jnp.float32).astype(jnp.bfloat16)
            )
        attended = jnp.concatenate(heads, axis=1)
        out[...] = jnp.dot(attended, w[...], preferred_element_type=jnp.float32).astype(
            jnp.bfloat16
        )


def attend(half, info, sinks, slopes, q, k, v, halo, w, rows, blocks):
    group = sinks.shape[0]
    width = w.shape[1]
    tokens = k.shape[0]
    out = [jax.ShapeDtypeStruct((rows, width), jnp.bfloat16)] * blocks
    return call(
        functools.partial(attend_body, half=half, rows=rows, group=group),
        out,
        (info, sinks, slopes, q, k, v, halo, w),
        [SMEM] * 3 + [VMEM] * 5,
        2 * blocks * rows * w.shape[0] * width,
        [pltpu.VMEM((tokens + WINDOW, HEAD), jnp.bfloat16)] * 2,
        name=f"attend_{half}",
    )


def norm_body(stream, own, left, right, gain, bias, out):
    total = (
        own[...].astype(jnp.float32)
        + left[...].astype(jnp.float32)
        + right[...].astype(jnp.float32)
    )
    value = deep_alpha * stream[...].astype(jnp.float32) + total
    mean = jnp.mean(value, axis=-1, keepdims=True)
    centred = value - mean
    spread = jnp.mean(jnp.square(centred), axis=-1, keepdims=True)
    out[...] = (centred * lax.rsqrt(spread + norm_eps) * gain[...] + bias[...]).astype(
        jnp.bfloat16
    )


def norm(stream, own, left, right, gain, bias, name):
    return call(
        norm_body,
        jax.ShapeDtypeStruct(stream.shape, jnp.bfloat16),
        (stream, own, left, right, gain, bias),
        [VMEM] * 6,
        20 * stream.size * 10,
        name=name,
    )


def ffn_body(place, *refs, rows, n_in, n_up, n_down):
    xs = refs[:n_in]
    ups = refs[n_in : n_in + n_up]
    downs = refs[n_in + n_up : n_in + n_up + n_down]
    outs = refs[n_in + n_up + n_down : 2 * n_in + n_up + n_down]
    up, down, sems = refs[2 * n_in + n_up + n_down :]
    z, y, c = place[0], place[1], place[2]
    up_at = [0, -1, -2, -3, 1, 2, 3]
    for side in range(2):
        core = (c + side) % 2
        pieces = ups[side * 9 : side * 9 + 9]
        for i, dz in enumerate(up_at):
            for j in range(Y):
                pltpu.make_async_copy(
                    pieces[i].at[j], up.at[(z + dz) % Z, (y + j) % Y, core], sems.at[0]
                ).start()
        for h in range(2):
            for j in range(Y // 2):
                pltpu.make_async_copy(
                    pieces[7 + h].at[j],
                    up.at[(z + Z // 2) % Z, (y + h * (Y // 2) + j) % Y, core],
                    sems.at[0],
                ).start()
    down_at = [0, -1, 1]
    for side in range(2):
        core = (c + side) % 2
        pieces = downs[side * 5 : side * 5 + 5]
        for i, dy in enumerate(down_at):
            for j in range(Z):
                pltpu.make_async_copy(
                    pieces[i].at[j], down.at[(z + j) % Z, (y + dy) % Y, core], sems.at[1]
                ).start()
        for h in range(2):
            for j in range(Z // 2):
                pltpu.make_async_copy(
                    pieces[3 + h].at[j],
                    down.at[(z + h * (Z // 2) + j) % Z, (y + Y // 2) % Y, core],
                    sems.at[1],
                ).start()
    width = up.shape[-1]
    x = jnp.concatenate([r[...] for r in xs], axis=0)
    pltpu.make_async_copy(up, up, sems.at[0]).wait()
    step = 512
    acts = []
    for n in range(0, width, step):
        w = up[:, :, :, :, n : n + step].reshape(-1, step)
        upward = jnp.dot(x, w, preferred_element_type=jnp.float32)
        acts.append(jnp.square(jnp.maximum(upward, 0.0)).astype(jnp.bfloat16))
    act = jnp.concatenate(acts, axis=1)
    pltpu.make_async_copy(down, down, sems.at[1]).wait()
    flat = down.reshape(-1, width)
    for n in range(0, flat.shape[0], step):
        part = lax.dot_general(
            act,
            flat[n : n + step],
            (((1,), (1,)), ((), ())),
            preferred_element_type=jnp.float32,
        ).astype(jnp.bfloat16)
        for i, out in enumerate(outs):
            out[:, n : n + step] = part[i * rows : (i + 1) * rows]


def ffn(place, xs, ups, downs, name):
    rows, width = xs[0].shape
    hidden = ups[0].shape[-1]
    per = ups[0].shape[1]
    out = [jax.ShapeDtypeStruct((rows, width), jnp.bfloat16)] * len(xs)
    return call(
        functools.partial(ffn_body, rows=rows, n_in=len(xs), n_up=len(ups), n_down=len(downs)),
        out,
        (place, *xs, *ups, *downs),
        [SMEM] + [VMEM] * len(xs) + [HBM] * (len(ups) + len(downs)),
        4 * len(xs) * rows * width * hidden,
        [
            pltpu.VMEM((Z, Y, 2, per, hidden), jnp.bfloat16),
            pltpu.VMEM((Z, Y, 2, per, hidden), jnp.bfloat16),
            pltpu.SemaphoreType.DMA((2,)),
        ],
        name=name,
    )


def gathered_up(shard):
    ahead = [y_move(shard, -k) for k in range(1, Y)]
    block = jnp.stack([shard, *ahead])
    down, up, far = ring(block, z_move, Z)
    own = down + up + far
    return own + [core_swap(p) for p in own]


def gathered_down(shard):
    down, up, far = ring(shard, z_move, Z)
    whole = jnp.concatenate(far, axis=0)
    block = jnp.stack([shard, *up, whole, *down[:0:-1]])
    down, up, far = ring(block, y_move, Y)
    own = down + up + far
    return own + [core_swap(p) for p in own]


def add(a, b):
    return (a.astype(jnp.float32) + b.astype(jnp.float32)).astype(jnp.bfloat16)


def scatter_sum(a, b):
    far_a = x_move(a[2], 1)
    left_a = x_move(a[3], -1)
    far_b = x_move(b[2], -1)
    right_a = x_move(add(a[1], far_a), 1)
    right_b = x_move(b[1], 1)
    left_b = x_move(add(b[3], far_b), -1)
    return (a[0], right_a, left_a), (b[0], right_b, left_b)


def spread_out(a, b):
    a_prev = x_move(a, 1)
    a_next = x_move(a, -1)
    b_next = x_move(b, -1)
    a_far = x_move(a_prev, 1)
    b_prev = x_move(b, 1)
    b_far = x_move(b_next, -1)
    return (a, a_next, a_far, a_prev), (b, b_next, b_far, b_prev)


def on_device(
    queries, keys, values, residual, sinks, out_weight, up_weight, down_weight, gains, biases
):
    tokens = queries.shape[0]
    own = residual.shape[0]
    rows = own // 2
    rank = lax.axis_index("tp")
    s = lax.axis_index("sp")
    place = jnp.stack([s // (2 * Y), s // 2 % Y, s % 2])

    tails = jnp.stack([keys[tokens - WINDOW :], values[tokens - WINDOW :]])
    halo = from_behind(tails, "sp", 1)
    ups = gathered_up(up_weight)
    downs = gathered_down(down_weight.T)

    heads = (jnp.arange(sinks.shape[0], dtype=jnp.int32) + rank * sinks.shape[0]).astype(
        jnp.float32
    )
    slopes = jnp.exp2(-8.0 * (heads + 1.0) / HEADS)
    info = jnp.stack([rank, s * tokens])
    shares = [
        attend(h, info, sinks, slopes, queries, keys, values, halo, out_weight, rows, tokens // own)
        for h in range(2)
    ]
    mix_a, mix_b = scatter_sum(*shares)
    gain0, bias0 = gains[:1], biases[:1]
    gain1, bias1 = gains[1:], biases[1:]
    norm_a = norm(residual[:rows], *mix_a, gain0, bias0, "norm0_a")
    norm_b = norm(residual[rows:], *mix_b, gain0, bias0, "norm0_b")
    all_a, all_b = spread_out(norm_a, norm_b)
    out_a = ffn(place, all_a, ups, downs, "ffn_a")
    out_b = ffn(place, all_b, ups, downs, "ffn_b")
    ffn_a, ffn_b = scatter_sum(out_a, out_b)
    done_a = norm(norm_a, *ffn_a, gain1, bias1, "norm1_a")
    done_b = norm(norm_b, *ffn_b, gain1, bias1, "norm1_b")
    return jnp.concatenate([done_a, done_b], axis=0)


def solution(mesh):
    return jax.shard_map(
        on_device,
        mesh=mesh,
        in_specs=(
            P("sp", "tp"),
            P("sp", "tp"),
            P("sp", "tp"),
            P(("sp", "tp"), None),
            P("tp"),
            P("tp", None),
            P("sp", "tp"),
            P("tp", "sp"),
            P(),
            P(),
        ),
        out_specs=P(("sp", "tp"), None),
        check_vma=False,
    )
```

```python
import functools

import jax
import jax.numpy as jnp
from jax import lax
from jax.experimental import pallas as pl
from jax.experimental.pallas import tpu as pltpu
from jax.sharding import PartitionSpec as P


HEADS = 12
HEAD = 128
WINDOW = 128
Y, Z = 4, 8

deep_alpha = 1.6817928
norm_eps = 1e-05
neg_big = -1e30


VMEM = pl.BlockSpec(memory_space=pltpu.VMEM)
SMEM = pl.BlockSpec(memory_space=pltpu.SMEM)
HBM = pl.BlockSpec(memory_space=pltpu.HBM)


def call(body, outs, args, specs, flops, mib, scratch=()):
    return pl.pallas_call(
        body,
        out_shape=outs,
        in_specs=specs,
        out_specs=jax.tree.map(lambda _: VMEM, outs),
        scratch_shapes=list(scratch),
        compiler_params=pltpu.CompilerParams(vmem_limit_bytes=mib * 2**20),
        cost_estimate=pl.CostEstimate(flops=flops, transcendentals=0, bytes_accessed=0),
    )(*args)


def sp_route(to):
    pairs = []
    for i in range(Z * Y * 2):
        z, y, c = to(i // (2 * Y), i // 2 % Y, i % 2)
        pairs.append((i, z % Z * 2 * Y + y % Y * 2 + c))
    return pairs


def z_first(block, flip=0):
    def to(z, y, c):
        return (z ^ 1 if c == flip else z + 2 * (z % 2) - 1), y, c

    return lax.ppermute(block, "sp", sp_route(to))


def z_second(block):
    return z_first(block, 1)


def y_first(block, flip=0):
    return lax.ppermute(block, "sp", sp_route(lambda z, y, c: (z, y ^ (1 if c == flip else 3), c)))


def y_second(block):
    return y_first(block, 1)


def x_first(block, flip=0):
    count = lax.axis_size("tp")
    pairs = []
    for i in range(lax.axis_size("sp") * count):
        x, c = i % count, i // count % 2
        pairs.append((i, i - x + (x ^ (1 if c == flip else 3))))
    return lax.ppermute(block, ("sp", "tp"), pairs)


def x_second(block):
    return x_first(block, 1)


def swap(block):
    return lax.ppermute(block, "sp", sp_route(lambda z, y, c: (z, y, 1 - c)))


def from_behind(block, axis, distance):
    devices = range(lax.axis_size(axis))
    route = [(i - distance, i) for i in devices if i - distance in devices]
    return lax.ppermute(block, axis, route)


def z_at(z, core, i):
    sign = (1 - 2 * (z % 2)) * (1 - 2 * core)
    steps = (0, sign, 2 * sign, 3 * sign, -sign, -2 * sign, -3 * sign, 4)
    return (z + steps[i] + Z) % Z


def y_at(y, core, j):
    one = 1 + 2 * core
    return y ^ (0, one, one ^ 2, 2)[j]


def stack_body(place, *refs, n_in, along_z):
    outs = refs[n_in:]
    width = outs[0].shape[2]
    for i, ref in enumerate(refs[:n_in]):
        if along_z:
            at = z_at(place[0], place[2], i)
        else:
            at = y_at(place[1], place[2], i)
        for n, out in enumerate(outs):
            out[at] = ref[:, n * width : (n + 1) * width]


def stack(place, pieces, along_z, parts):
    rows, width = pieces[0].shape
    out = [jax.ShapeDtypeStruct((len(pieces), rows, width // parts), pieces[0].dtype)] * parts
    return call(
        functools.partial(stack_body, n_in=len(pieces), along_z=along_z),
        out,
        (place, *pieces),
        [SMEM] + [VMEM] * len(pieces),
        4 * 10**8,
        4,
    )


def z_ring(block):
    first, second = [z_first(block)], [z_second(block)]
    for _ in range(2):
        f, s = z_first(second[-1]), z_second(first[-1])
        first.append(f)
        second.append(s)
    return [block, *first, *second, z_first(second[-1])]


def y_ring(block):
    first, second = y_first(block), y_second(block)
    return [block, first, second, y_first(second)]


def gathered_up(place, shard):
    left, right = stack(place, y_ring(shard), False, 2)
    left, right = z_ring(left), z_ring(right)
    return [*left, *right, *(swap(p) for p in left), *(swap(p) for p in right)]


def gathered_down(place, shard):
    own = y_ring(stack(place, z_ring(shard), True, 1)[0])
    return own + [swap(p) for p in own]


def attend_body(info, sinks, slopes, q_in, k, v, halo, w_in, *rest, rows):
    outs, (k_ext, v_ext, q, w, sems, logits, weights, attended) = rest[:-8], rest[-8:]
    tokens = k.shape[0]
    copies = [
        pltpu.make_async_copy(src, dst, sems.at[i])
        for i, (src, dst) in enumerate(
            (
                (k, k_ext.at[WINDOW : WINDOW + tokens]),
                (q_in, q),
                (halo.at[0], k_ext.at[:WINDOW]),
                (v, v_ext.at[WINDOW : WINDOW + tokens]),
                (halo.at[1], v_ext.at[:WINDOW]),
                (w_in, w),
            )
        )
    ]
    for copy in copies:
        copy.start()
    rank, offset, core = info[0], info[1], info[2]
    one = 1 + 2 * core
    plan = [(rel, half) for rel in (2, one, one ^ 2, 0) for half in range(2)]
    for copy in copies[:3]:
        copy.wait()
    group = sinks.shape[0]
    span = rows + WINDOW

    def start_of(rel, half):
        return pl.multiple_of((rank ^ rel) * (2 * rows) + half * rows, rows)

    for at, (rel, half) in enumerate(plan):
        start = start_of(rel, half)
        key = k_ext[pl.ds(start, span), :]
        query = jnp.concatenate(
            [q[pl.ds(start, rows), g * HEAD : (g + 1) * HEAD] for g in range(group)], axis=0
        )
        logits[at] = lax.dot_general(
            query, key, (((1,), (1,)), ((), ())), preferred_element_type=jnp.float32
        )
    shape = (rows, span)
    q_index = lax.broadcasted_iota(jnp.int32, shape, 0)
    k_index = lax.broadcasted_iota(jnp.int32, shape, 1)
    dist = q_index + WINDOW - k_index
    in_window = (dist >= 0) & (dist < WINDOW)
    dist_f = dist.astype(jnp.float32)
    bias = [jnp.where(in_window, slopes[g] * dist_f, -neg_big) for g in range(group)]
    for at, (rel, half) in enumerate(plan):
        ahead = WINDOW - offset - start_of(rel, half)
        for g in range(group):
            part = logits[at, g * rows : (g + 1) * rows, :] * HEAD ** (-0.5) - bias[g]
            part = jnp.where(k_index < ahead, neg_big, part)
            top = jnp.maximum(jnp.max(part, axis=-1, keepdims=True), sinks[g])
            probs = jnp.exp(part - top)
            denom = jnp.sum(probs, axis=-1, keepdims=True) + jnp.exp(sinks[g] - top)
            weights[at, g * rows : (g + 1) * rows, :] = (probs * (1.0 / denom)).astype(
                jnp.bfloat16
            )
    for copy in copies[3:]:
        copy.wait()
    for at, (rel, half) in enumerate(plan):
        val = v_ext[pl.ds(start_of(rel, half), span), :]
        mixed = jnp.dot(weights[at], val, preferred_element_type=jnp.float32).astype(jnp.bfloat16)
        for g in range(group):
            attended[at * rows : (at + 1) * rows, g * HEAD : (g + 1) * HEAD] = mixed[
                g * rows : (g + 1) * rows
            ]
    step = 256

    def project(n, carry):
        cols = pl.ds(pl.multiple_of(n * step, step), step)
        mix = jnp.dot(attended[...], w[:, cols], preferred_element_type=jnp.float32).astype(
            jnp.bfloat16
        )
        at = 0
        for out in outs:
            out[:, cols] = mix[at : at + out.shape[0]]
            at += out.shape[0]
        return carry

    lax.fori_loop(0, w.shape[1] // step, project, 0)


def attend(info, sinks, slopes, q, k, v, halo, w, rows):
    width = w.shape[1]
    ext = pltpu.VMEM((k.shape[0] + WINDOW, HEAD), jnp.bfloat16)
    tall, span = sinks.shape[0] * rows, rows + WINDOW
    return call(
        functools.partial(attend_body, rows=rows),
        [jax.ShapeDtypeStruct((2 * rows, width), jnp.bfloat16)] * 4,
        (info, sinks, slopes, q, k, v, halo, w),
        [SMEM] * 3 + [HBM] * 5,
        6 * 10**9,
        54,
        [
            ext,
            ext,
            pltpu.VMEM(q.shape, jnp.bfloat16),
            pltpu.VMEM(w.shape, jnp.bfloat16),
            pltpu.SemaphoreType.DMA((6,)),
            pltpu.VMEM((8, tall, span), jnp.float32),
            pltpu.VMEM((8, tall, span), jnp.bfloat16),
            pltpu.VMEM((8 * rows, w.shape[0]), jnp.bfloat16),
        ],
    )


def norm(stream, gain, bias, *shares):
    mix = functools.reduce(lambda a, b: a + b, (p.astype(jnp.float32) for p in shares))
    value = deep_alpha * stream.astype(jnp.float32) + mix
    mean = jnp.mean(value, axis=-1, keepdims=True)
    spread = jnp.mean(jnp.square(value - mean), axis=-1, keepdims=True)
    return ((value - mean) * lax.rsqrt(spread + norm_eps) * gain + bias).astype(jnp.bfloat16)


def place_weights(place, ups, downs, up, down, sems):
    z, y, c = place[0], place[1], place[2]
    half = up.shape[-1] // 2

    def start_up():
        for side in range(2):
            core = c ^ side
            for n in range(2):
                for i in range(Z):
                    pltpu.make_async_copy(
                        ups[(2 * side + n) * Z + i],
                        up.at[z_at(z, core, i), :, core, :, n * half : (n + 1) * half],
                        sems.at[0],
                    ).start()

    def start_down():
        for side in range(2):
            core = c ^ side
            for j in range(Y):
                pltpu.make_async_copy(
                    downs[side * Y + j], down.at[:, y_at(y, core, j), core], sems.at[1]
                ).start()

    return start_up, start_down


def ffn_rows(xs, outs, up, down, act, ready_up, ready_down):
    step = 256
    width = up.shape[-1]
    x = jnp.concatenate([r[...] for r in xs], axis=0) if len(xs) > 1 else xs[0][...]
    ready_up()

    def raise_(n, carry):
        cols = pl.ds(pl.multiple_of(n * step, step), step)
        w = up[:, :, :, :, cols].reshape(-1, step)
        upward = jnp.dot(x, w, preferred_element_type=jnp.float32)
        act[:, cols] = jnp.square(jnp.maximum(upward, 0.0)).astype(jnp.bfloat16)
        return carry

    lax.fori_loop(0, width // step, raise_, 0)
    ready_down()
    a = act[...]
    z_step = step // (down.shape[1] * down.shape[2] * down.shape[3])

    def lower(n, carry):
        w = down[pl.ds(n * z_step, z_step)].reshape(step, width)
        part = lax.dot_general(
            a, w, (((1,), (1,)), ((), ())), preferred_element_type=jnp.float32
        ).astype(jnp.bfloat16)
        cols = pl.ds(pl.multiple_of(n * step, step), step)
        at = 0
        for out in outs:
            out[:, cols] = part[at : at + out.shape[0]]
            at += out.shape[0]
        return carry

    lax.fori_loop(0, down.shape[0] // z_step, lower, 0)


def ffn_body(place, *refs, n_in, n_out, n_up, n_down):
    xs, refs = refs[:n_in], refs[n_in:]
    ups, downs, refs = refs[:n_up], refs[n_up : n_up + n_down], refs[n_up + n_down :]
    outs, (up, down, act, sems) = refs[:n_out], refs[n_out:]
    start_up, start_down = place_weights(place, ups, downs, up, down, sems)

    def ready_up():
        pltpu.make_async_copy(up, up, sems.at[0]).wait()
        start_down()

    def ready_down():
        pltpu.make_async_copy(down, down, sems.at[1]).wait()

    start_up()
    ffn_rows(xs, outs, up, down, act, ready_up, ready_down)


def ffn(place, xs, counts, ups, downs):
    rows = sum(x.shape[0] for x in xs)
    width = xs[0].shape[1]
    hidden = downs[0].shape[-1]
    out, at = [], 0
    for n in counts:
        height = sum(x.shape[0] for x in xs[at : at + n])
        out.append(jax.ShapeDtypeStruct((height, width), jnp.bfloat16))
        at += n
    weights = pltpu.VMEM((Z, Y, 2, width // (Z * Y * 2), hidden), jnp.bfloat16)
    return call(
        functools.partial(ffn_body, n_in=len(xs), n_out=len(counts), n_up=len(ups), n_down=len(downs)),
        out,
        (place, *xs, *ups, *downs),
        [SMEM] + [VMEM] * len(xs) + [HBM] * (len(ups) + len(downs)),
        4 * rows * width * hidden,
        28,
        [weights, weights, pltpu.VMEM((rows, hidden), jnp.bfloat16), pltpu.SemaphoreType.DMA((2,))],
    )


def add(a, b):
    return (a.astype(jnp.float32) + b.astype(jnp.float32)).astype(jnp.bfloat16)


def on_device(
    queries, keys, values, residual, sinks, out_weight, up_weight, down_weight, gains, biases
):
    tokens = queries.shape[0]
    rows = residual.shape[0] // 2
    rank = lax.axis_index("tp")
    s = lax.axis_index("sp")
    place = jnp.stack([s // (2 * Y), s // 2 % Y, s % 2])

    tails = jnp.stack([keys[tokens - WINDOW :], values[tokens - WINDOW :]])
    halo = from_behind(tails, "sp", 1)
    ups = gathered_up(place, up_weight)
    downs = gathered_down(place, down_weight.T)

    heads = (jnp.arange(sinks.shape[0], dtype=jnp.int32) + rank * sinks.shape[0]).astype(
        jnp.float32
    )
    slopes = jnp.exp2(-8.0 * (heads + 1.0) / HEADS)
    info = jnp.stack([rank, s * tokens, s % 2])
    far, first, second, own = attend(
        info, sinks, slopes, queries, keys, values, halo, out_weight, rows
    )
    from_far = x_first(far)
    from_first = x_first(first)
    from_second = x_second(add(second, from_far))
    normed = norm(residual, gains[0], biases[0], own, from_first, from_second)
    first = x_first(normed)
    second = [x_second(normed[:rows]), x_second(normed[rows:])]
    far = [x_first(second[0]), x_first(second[1])]
    far, first = ffn(place, (*far, first), (2, 1), ups, downs)
    from_far = x_first(far)
    from_first = x_first(first)
    second, own = ffn(place, (*second, normed), (2, 1), ups, downs)
    from_second = x_second(add(second, from_far))
    return norm(normed, gains[1], biases[1], own, from_first, from_second)


def solution(mesh):
    return jax.shard_map(
        on_device,
        mesh=mesh,
        in_specs=(
            P("sp", "tp"),
            P("sp", "tp"),
            P("sp", "tp"),
            P(("sp", "tp"), None),
            P("tp"),
            P("tp", None),
            P("sp", "tp"),
            P("tp", "sp"),
            P(),
            P(),
        ),
        out_specs=P(("sp", "tp"), None),
        check_vma=False,
    )
```

```python
import functools

import jax
import jax.numpy as jnp
from jax import lax
from jax.experimental import pallas as pl
from jax.experimental.pallas import tpu as pltpu
from jax.sharding import PartitionSpec as P


HEADS = 12
HEAD = 128
WINDOW = 128
Y, Z = 4, 8
NEAR = 1792

deep_alpha = 1.6817928
norm_eps = 1e-05
neg_big = -1e30


VMEM = pl.BlockSpec(memory_space=pltpu.VMEM)
SMEM = pl.BlockSpec(memory_space=pltpu.SMEM)
HBM = pl.BlockSpec(memory_space=pltpu.HBM)


def call(body, outs, args, specs, flops, mib, scratch=()):
    return pl.pallas_call(
        body,
        out_shape=outs,
        in_specs=specs,
        out_specs=jax.tree.map(lambda _: VMEM, outs),
        scratch_shapes=list(scratch),
        compiler_params=pltpu.CompilerParams(vmem_limit_bytes=mib * 2**20),
        cost_estimate=pl.CostEstimate(flops=flops, transcendentals=0, bytes_accessed=0),
    )(*args)


def sp_route(to):
    pairs = []
    for i in range(Z * Y * 2):
        z, y, c = to(i // (2 * Y), i // 2 % Y, i % 2)
        pairs.append((i, z % Z * 2 * Y + y % Y * 2 + c))
    return pairs


def z_first(block, flip=0):
    def to(z, y, c):
        return (z ^ 1 if c == flip else z + 2 * (z % 2) - 1), y, c

    return lax.ppermute(block, "sp", sp_route(to))


def z_second(block):
    return z_first(block, 1)


def y_first(block, flip=0):
    return lax.ppermute(block, "sp", sp_route(lambda z, y, c: (z, y ^ (1 if c == flip else 3), c)))


def y_second(block):
    return y_first(block, 1)


def x_first(block, flip=0):
    count = lax.axis_size("tp")
    pairs = []
    for i in range(lax.axis_size("sp") * count):
        x, c = i % count, i // count % 2
        pairs.append((i, i - x + (x ^ (1 if c == flip else 3))))
    return lax.ppermute(block, ("sp", "tp"), pairs)


def x_second(block):
    return x_first(block, 1)


def swap(block):
    return lax.ppermute(block, "sp", sp_route(lambda z, y, c: (z, y, 1 - c)))


def from_behind(block, axis, distance):
    devices = range(lax.axis_size(axis))
    route = [(i - distance, i) for i in devices if i - distance in devices]
    return lax.ppermute(block, axis, route)


def z_at(z, core, i):
    sign = (1 - 2 * (z % 2)) * (1 - 2 * core)
    steps = (0, sign, 2 * sign, 3 * sign, -sign, -2 * sign, -3 * sign, 4)
    return (z + steps[i] + Z) % Z


def y_at(y, core, j):
    one = 1 + 2 * core
    return y ^ (0, one, one ^ 2, 2)[j]


def stack_body(place, *refs, n_in, along_z):
    out = refs[n_in]
    for i, ref in enumerate(refs[:n_in]):
        if along_z:
            at = z_at(place[0], place[2], i)
        else:
            at = y_at(place[1], place[2], i)
        out[at] = ref[:, : out.shape[2]]


def stack(place, pieces, along_z, width):
    rows = pieces[0].shape[0]
    return call(
        functools.partial(stack_body, n_in=len(pieces), along_z=along_z),
        jax.ShapeDtypeStruct((len(pieces), rows, width), pieces[0].dtype),
        (place, *pieces),
        [SMEM] + [VMEM] * len(pieces),
        4 * 10**8,
        6,
    )


def z_ring(block):
    first, second = [z_first(block)], [z_second(block)]
    for _ in range(2):
        f, s = z_first(second[-1]), z_second(first[-1])
        first.append(f)
        second.append(s)
    return [block, *first, *second, z_first(second[-1])]


def y_ring(block):
    first, second = y_first(block), y_second(block)
    return [block, first, second, y_first(second)]


def gathered_up(place, shard):
    own = z_ring(stack(place, y_ring(shard), False, NEAR))
    return own + [swap(p) for p in own]


def gathered_down(place, shard):
    own = y_ring(stack(place, z_ring(shard), True, shard.shape[1]))
    return own + [swap(p) for p in own]


def attend_body(info, sinks, q_in, k, v, halo, w_in, *rest, rows):
    outs, (k_ext, v_ext, q, w, sems, logits, weights, attended) = rest[:-8], rest[-8:]
    tokens = k.shape[0]
    copies = [
        pltpu.make_async_copy(src, dst, sems.at[i])
        for i, (src, dst) in enumerate(
            (
                (k, k_ext.at[WINDOW : WINDOW + tokens]),
                (q_in, q),
                (halo.at[0], k_ext.at[:WINDOW]),
                (v, v_ext.at[WINDOW : WINDOW + tokens]),
                (halo.at[1], v_ext.at[:WINDOW]),
                (w_in, w),
            )
        )
    ]
    for copy in copies:
        copy.start()
    rank, offset, core = info[0], info[1], info[2]
    one = 1 + 2 * core
    plan = [(rel, half) for rel in (2, one, one ^ 2, 0) for half in range(2)]
    for copy in copies[:3]:
        copy.wait()
    group = sinks.shape[0]
    span = rows + WINDOW

    def start_of(rel, half):
        return pl.multiple_of((rank ^ rel) * (2 * rows) + half * rows, rows)

    for at, (rel, half) in enumerate(plan):
        start = start_of(rel, half)
        key = k_ext[pl.ds(start, span), :]
        query = jnp.concatenate(
            [q[pl.ds(start, rows), g * HEAD : (g + 1) * HEAD] for g in range(group)], axis=0
        )
        logits[at] = lax.dot_general(
            query, key, (((1,), (1,)), ((), ())), preferred_element_type=jnp.float32
        )
    shape = (rows, span)
    q_index = lax.broadcasted_iota(jnp.int32, shape, 0)
    k_index = lax.broadcasted_iota(jnp.int32, shape, 1)
    dist = q_index + WINDOW - k_index
    in_window = (dist >= 0) & (dist < WINDOW)
    dist_f = dist.astype(jnp.float32)
    bias = []
    for g in range(group):
        head = jnp.full(shape, rank * group + g, jnp.int32).astype(jnp.float32)
        slope = jnp.exp2(-8.0 * (head + 1.0) / HEADS)
        bias.append(jnp.where(in_window, slope * dist_f, -neg_big))
    for at, (rel, half) in enumerate(plan):
        ahead = WINDOW - offset - start_of(rel, half)
        for g in range(group):
            part = logits[at, g * rows : (g + 1) * rows, :] * HEAD ** (-0.5) - bias[g]
            part = jnp.where(k_index < ahead, neg_big, part)
            top = jnp.maximum(jnp.max(part, axis=-1, keepdims=True), sinks[g])
            probs = jnp.exp(part - top)
            denom = jnp.sum(probs, axis=-1, keepdims=True) + jnp.exp(sinks[g] - top)
            weights[at, g * rows : (g + 1) * rows, :] = (probs * (1.0 / denom)).astype(
                jnp.bfloat16
            )
    for copy in copies[3:]:
        copy.wait()
    for at, (rel, half) in enumerate(plan):
        val = v_ext[pl.ds(start_of(rel, half), span), :]
        mixed = jnp.dot(weights[at], val, preferred_element_type=jnp.float32).astype(jnp.bfloat16)
        for g in range(group):
            attended[at * rows : (at + 1) * rows, g * HEAD : (g + 1) * HEAD] = mixed[
                g * rows : (g + 1) * rows
            ]
    step = 256

    def project(n, carry):
        cols = pl.ds(pl.multiple_of(n * step, step), step)
        mix = jnp.dot(attended[...], w[:, cols], preferred_element_type=jnp.float32).astype(
            jnp.bfloat16
        )
        at = 0
        for out in outs:
            out[:, cols] = mix[at : at + out.shape[0]]
            at += out.shape[0]
        return carry

    lax.fori_loop(0, w.shape[1] // step, project, 0)


def attend(info, sinks, q, k, v, halo, w, rows):
    width = w.shape[1]
    ext = pltpu.VMEM((k.shape[0] + WINDOW, HEAD), jnp.bfloat16)
    tall, span = sinks.shape[0] * rows, rows + WINDOW
    return call(
        functools.partial(attend_body, rows=rows),
        [jax.ShapeDtypeStruct((2 * rows, width), jnp.bfloat16)] * 4,
        (info, sinks, q, k, v, halo, w),
        [SMEM] * 2 + [HBM] * 5,
        6 * 10**9,
        54,
        [
            ext,
            ext,
            pltpu.VMEM(q.shape, jnp.bfloat16),
            pltpu.VMEM(w.shape, jnp.bfloat16),
            pltpu.SemaphoreType.DMA((6,)),
            pltpu.VMEM((8, tall, span), jnp.float32),
            pltpu.VMEM((8, tall, span), jnp.bfloat16),
            pltpu.VMEM((8 * rows, w.shape[0]), jnp.bfloat16),
        ],
    )


def norm(stream, gain, bias, *shares):
    mix = functools.reduce(lambda a, b: a + b, (p.astype(jnp.float32) for p in shares))
    value = deep_alpha * stream.astype(jnp.float32) + mix
    mean = jnp.mean(value, axis=-1, keepdims=True)
    spread = jnp.mean(jnp.square(value - mean), axis=-1, keepdims=True)
    return ((value - mean) * lax.rsqrt(spread + norm_eps) * gain + bias).astype(jnp.bfloat16)


def place_weights(place, ups, downs, up, down, sems):
    z, y, c = place[0], place[1], place[2]
    hidden, near = up.shape[-1], ups[0].shape[-1]

    def start_up():
        for side in range(2):
            core = c ^ side
            for j in range(Y):
                pltpu.make_async_copy(
                    downs[side * Y + j].at[:, :, hidden:],
                    up.at[:, y_at(y, core, j), core, :, near:],
                    sems.at[0],
                ).start()
            for i in range(Z):
                pltpu.make_async_copy(
                    ups[side * Z + i], up.at[z_at(z, core, i), :, core, :, :near], sems.at[0]
                ).start()

    def start_down():
        for side in range(2):
            core = c ^ side
            for j in range(Y):
                pltpu.make_async_copy(
                    downs[side * Y + j].at[:, :, :hidden],
                    down.at[:, y_at(y, core, j), core],
                    sems.at[1],
                ).start()

    return start_up, start_down


def ffn_rows(xs, outs, up, down, act, ready_up, ready_down):
    step = 256
    width = up.shape[-1]
    x = jnp.concatenate([r[...] for r in xs], axis=0) if len(xs) > 1 else xs[0][...]
    ready_up()

    def raise_(n, carry):
        cols = pl.ds(pl.multiple_of(n * step, step), step)
        w = up[:, :, :, :, cols].reshape(-1, step)
        upward = jnp.dot(x, w, preferred_element_type=jnp.float32)
        act[:, cols] = jnp.square(jnp.maximum(upward, 0.0)).astype(jnp.bfloat16)
        return carry

    lax.fori_loop(0, width // step, raise_, 0)
    ready_down()
    a = act[...]
    z_step = step // (down.shape[1] * down.shape[2] * down.shape[3])

    def lower(n, carry):
        w = down[pl.ds(n * z_step, z_step)].reshape(step, width)
        part = lax.dot_general(
            a, w, (((1,), (1,)), ((), ())), preferred_element_type=jnp.float32
        ).astype(jnp.bfloat16)
        cols = pl.ds(pl.multiple_of(n * step, step), step)
        at = 0
        for out in outs:
            out[:, cols] = part[at : at + out.shape[0]]
            at += out.shape[0]
        return carry

    lax.fori_loop(0, down.shape[0] // z_step, lower, 0)


def ffn_body(place, *refs, n_in, n_out, n_up, n_down):
    xs, refs = refs[:n_in], refs[n_in:]
    ups, downs, refs = refs[:n_up], refs[n_up : n_up + n_down], refs[n_up + n_down :]
    outs, (up, down, act, sems) = refs[:n_out], refs[n_out:]
    start_up, start_down = place_weights(place, ups, downs, up, down, sems)

    def ready_up():
        pltpu.make_async_copy(up, up, sems.at[0]).wait()
        start_down()

    def ready_down():
        pltpu.make_async_copy(down, down, sems.at[1]).wait()

    start_up()
    ffn_rows(xs, outs, up, down, act, ready_up, ready_down)


def ffn(place, xs, counts, ups, downs, hidden):
    rows = sum(x.shape[0] for x in xs)
    width = xs[0].shape[1]
    out, at = [], 0
    for n in counts:
        height = sum(x.shape[0] for x in xs[at : at + n])
        out.append(jax.ShapeDtypeStruct((height, width), jnp.bfloat16))
        at += n
    weights = pltpu.VMEM((Z, Y, 2, width // (Z * Y * 2), hidden), jnp.bfloat16)
    return call(
        functools.partial(ffn_body, n_in=len(xs), n_out=len(counts), n_up=len(ups), n_down=len(downs)),
        out,
        (place, *xs, *ups, *downs),
        [SMEM] + [VMEM] * len(xs) + [HBM] * (len(ups) + len(downs)),
        4 * rows * width * hidden,
        28,
        [weights, weights, pltpu.VMEM((rows, hidden), jnp.bfloat16), pltpu.SemaphoreType.DMA((2,))],
    )


def add(a, b):
    return (a.astype(jnp.float32) + b.astype(jnp.float32)).astype(jnp.bfloat16)


def on_device(
    queries, keys, values, residual, sinks, out_weight, up_weight, down_weight, gains, biases
):
    tokens = queries.shape[0]
    rows = residual.shape[0] // 2
    hidden = up_weight.shape[1]
    rank = lax.axis_index("tp")
    s = lax.axis_index("sp")
    place = jnp.stack([s // (2 * Y), s // 2 % Y, s % 2])

    tails = jnp.stack([keys[tokens - WINDOW :], values[tokens - WINDOW :]])
    halo = from_behind(tails, "sp", 1)
    ups = gathered_up(place, up_weight)
    downs = gathered_down(
        place, jnp.concatenate([down_weight.T, up_weight[:, NEAR:]], axis=1)
    )

    info = jnp.stack([rank, s * tokens, s % 2])
    far, first, second, own = attend(info, sinks, queries, keys, values, halo, out_weight, rows)
    from_far = x_first(far)
    from_first = x_first(first)
    from_second = x_second(add(second, from_far))
    normed = norm(residual, gains[0], biases[0], own, from_first, from_second)
    first = x_first(normed)
    second = [x_second(normed[:rows]), x_second(normed[rows:])]
    far = [x_first(second[0]), x_first(second[1])]
    far, first = ffn(place, (*far, first), (2, 1), ups, downs, hidden)
    from_far = x_first(far)
    from_first = x_first(first)
    second, own = ffn(place, (*second, normed), (2, 1), ups, downs, hidden)
    from_second = x_second(add(second, from_far))
    return norm(normed, gains[1], biases[1], own, from_first, from_second)


def solution(mesh):
    return jax.shard_map(
        on_device,
        mesh=mesh,
        in_specs=(
            P("sp", "tp"),
            P("sp", "tp"),
            P("sp", "tp"),
            P(("sp", "tp"), None),
            P("tp"),
            P("tp", None),
            P("sp", "tp"),
            P("tp", "sp"),
            P(),
            P(),
        ),
        out_specs=P(("sp", "tp"), None),
        check_vma=False,
    )
```

```python
import functools

import jax
import jax.numpy as jnp
from jax import lax
from jax.experimental import pallas as pl
from jax.experimental.pallas import tpu as pltpu
from jax.sharding import PartitionSpec as P


HEADS = 12
HEAD = 128
WINDOW = 128
Y, Z = 4, 8

deep_alpha = 1.6817928
norm_eps = 1e-05
neg_big = -1e30


VMEM = pl.BlockSpec(memory_space=pltpu.VMEM)
SMEM = pl.BlockSpec(memory_space=pltpu.SMEM)
HBM = pl.BlockSpec(memory_space=pltpu.HBM)


def call(body, outs, args, specs, flops, mib, scratch=()):
    return pl.pallas_call(
        body,
        out_shape=outs,
        in_specs=specs,
        out_specs=jax.tree.map(lambda _: VMEM, outs),
        scratch_shapes=list(scratch),
        compiler_params=pltpu.CompilerParams(vmem_limit_bytes=mib * 2**20),
        cost_estimate=pl.CostEstimate(flops=flops, transcendentals=0, bytes_accessed=0),
    )(*args)


def sp_route(to):
    pairs = []
    for i in range(Z * Y * 2):
        z, y, c = to(i // (2 * Y), i // 2 % Y, i % 2)
        pairs.append((i, z % Z * 2 * Y + y % Y * 2 + c))
    return pairs


def z_first(block, flip=0):
    def to(z, y, c):
        return (z ^ 1 if c == flip else z + 2 * (z % 2) - 1), y, c

    return lax.ppermute(block, "sp", sp_route(to))


def z_second(block):
    return z_first(block, 1)


def y_first(block, flip=0):
    return lax.ppermute(block, "sp", sp_route(lambda z, y, c: (z, y ^ (1 if c == flip else 3), c)))


def y_second(block):
    return y_first(block, 1)


def x_first(block, flip=0):
    count = lax.axis_size("tp")
    pairs = []
    for i in range(lax.axis_size("sp") * count):
        x, c = i % count, i // count % 2
        pairs.append((i, i - x + (x ^ (1 if c == flip else 3))))
    return lax.ppermute(block, ("sp", "tp"), pairs)


def x_second(block):
    return x_first(block, 1)


def swap(block):
    return lax.ppermute(block, "sp", sp_route(lambda z, y, c: (z, y, 1 - c)))


def from_behind(block, axis, distance):
    devices = range(lax.axis_size(axis))
    route = [(i - distance, i) for i in devices if i - distance in devices]
    return lax.ppermute(block, axis, route)


def z_at(z, core, i):
    sign = (1 - 2 * (z % 2)) * (1 - 2 * core)
    steps = (0, sign, 2 * sign, 3 * sign, -sign, -2 * sign, -3 * sign, 4)
    return (z + steps[i] + Z) % Z


def y_at(y, core, j):
    one = 1 + 2 * core
    return y ^ (0, one, one ^ 2, 2)[j]


def stack_body(place, *refs, n_in, along_z):
    out = refs[n_in]
    for i, ref in enumerate(refs[:n_in]):
        if along_z:
            at = z_at(place[0], place[2], i)
        else:
            at = y_at(place[1], place[2], i)
        out[at] = ref[...]


def stack(place, pieces, along_z):
    rows, width = pieces[0].shape
    return call(
        functools.partial(stack_body, n_in=len(pieces), along_z=along_z),
        jax.ShapeDtypeStruct((len(pieces), rows, width), pieces[0].dtype),
        (place, *pieces),
        [SMEM] + [VMEM] * len(pieces),
        4 * 10**8,
        6,
    )


def z_ring(block):
    first, second = [z_first(block)], [z_second(block)]
    for _ in range(2):
        f, s = z_first(second[-1]), z_second(first[-1])
        first.append(f)
        second.append(s)
    return [block, *first, *second, z_first(second[-1])]


def y_ring(block):
    first, second = y_first(block), y_second(block)
    return [block, first, second, y_first(second)]


def gathered_up(place, shard):
    own = z_ring(stack(place, y_ring(shard), False))
    return own + [swap(p) for p in own]


def gathered_down(place, shard):
    own = y_ring(stack(place, z_ring(shard), True))
    return own + [swap(p) for p in own]


def attend_body(info, sinks, q_in, k, v, halo, w_in, *rest, rows):
    outs, (k_ext, v_ext, q, w, sems, logits, weights, attended) = rest[:-8], rest[-8:]
    tokens = k.shape[0]
    copies = [
        pltpu.make_async_copy(src, dst, sems.at[i])
        for i, (src, dst) in enumerate(
            (
                (k, k_ext.at[WINDOW : WINDOW + tokens]),
                (q_in, q),
                (halo.at[0], k_ext.at[:WINDOW]),
                (v, v_ext.at[WINDOW : WINDOW + tokens]),
                (halo.at[1], v_ext.at[:WINDOW]),
                (w_in, w),
            )
        )
    ]
    for copy in copies:
        copy.start()
    rank, offset, core = info[0], info[1], info[2]
    one = 1 + 2 * core
    plan = [(rel, half) for rel in (2, one, one ^ 2, 0) for half in range(2)]
    for copy in copies[:3]:
        copy.wait()
    group = sinks.shape[0]
    span = rows + WINDOW

    def start_of(rel, half):
        return pl.multiple_of((rank ^ rel) * (2 * rows) + half * rows, rows)

    for at, (rel, half) in enumerate(plan):
        start = start_of(rel, half)
        key = k_ext[pl.ds(start, span), :]
        query = jnp.concatenate(
            [q[pl.ds(start, rows), g * HEAD : (g + 1) * HEAD] for g in range(group)], axis=0
        )
        logits[at] = lax.dot_general(
            query, key, (((1,), (1,)), ((), ())), preferred_element_type=jnp.float32
        )
    shape = (rows, span)
    q_index = lax.broadcasted_iota(jnp.int32, shape, 0)
    k_index = lax.broadcasted_iota(jnp.int32, shape, 1)
    dist = q_index + WINDOW - k_index
    in_window = (dist >= 0) & (dist < WINDOW)
    dist_f = dist.astype(jnp.float32)
    bias = []
    for g in range(group):
        head = jnp.full(shape, rank * group + g, jnp.int32).astype(jnp.float32)
        slope = jnp.exp2(-8.0 * (head + 1.0) / HEADS)
        bias.append(jnp.where(in_window, slope * dist_f, -neg_big))
    for at, (rel, half) in enumerate(plan):
        ahead = WINDOW - offset - start_of(rel, half)
        for g in range(group):
            part = logits[at, g * rows : (g + 1) * rows, :] * HEAD ** (-0.5) - bias[g]
            part = jnp.where(k_index < ahead, neg_big, part)
            top = jnp.maximum(jnp.max(part, axis=-1, keepdims=True), sinks[g])
            probs = jnp.exp(part - top)
            denom = jnp.sum(probs, axis=-1, keepdims=True) + jnp.exp(sinks[g] - top)
            weights[at, g * rows : (g + 1) * rows, :] = (probs * (1.0 / denom)).astype(
                jnp.bfloat16
            )
    for copy in copies[3:]:
        copy.wait()
    for at, (rel, half) in enumerate(plan):
        val = v_ext[pl.ds(start_of(rel, half), span), :]
        mixed = jnp.dot(weights[at], val, preferred_element_type=jnp.float32).astype(jnp.bfloat16)
        for g in range(group):
            attended[at * rows : (at + 1) * rows, g * HEAD : (g + 1) * HEAD] = mixed[
                g * rows : (g + 1) * rows
            ]
    step = 512

    def project(n, carry):
        cols = pl.ds(pl.multiple_of(n * step, step), step)
        mix = jnp.dot(attended[...], w[:, cols], preferred_element_type=jnp.float32).astype(
            jnp.bfloat16
        )
        at = 0
        for out in outs:
            out[:, cols] = mix[at : at + out.shape[0]]
            at += out.shape[0]
        return carry

    lax.fori_loop(0, w.shape[1] // step, project, 0)


def attend(info, sinks, q, k, v, halo, w, rows):
    width = w.shape[1]
    ext = pltpu.VMEM((k.shape[0] + WINDOW, HEAD), jnp.bfloat16)
    tall, span = sinks.shape[0] * rows, rows + WINDOW
    return call(
        functools.partial(attend_body, rows=rows),
        [jax.ShapeDtypeStruct((2 * rows, width), jnp.bfloat16)] * 4,
        (info, sinks, q, k, v, halo, w),
        [SMEM] * 2 + [HBM] * 5,
        6 * 10**9,
        54,
        [
            ext,
            ext,
            pltpu.VMEM(q.shape, jnp.bfloat16),
            pltpu.VMEM(w.shape, jnp.bfloat16),
            pltpu.SemaphoreType.DMA((6,)),
            pltpu.VMEM((8, tall, span), jnp.float32),
            pltpu.VMEM((8, tall, span), jnp.bfloat16),
            pltpu.VMEM((8 * rows, w.shape[0]), jnp.bfloat16),
        ],
    )


def norm(stream, gain, bias, *shares):
    mix = functools.reduce(lambda a, b: a + b, (p.astype(jnp.float32) for p in shares))
    value = deep_alpha * stream.astype(jnp.float32) + mix
    mean = jnp.mean(value, axis=-1, keepdims=True)
    spread = jnp.mean(jnp.square(value - mean), axis=-1, keepdims=True)
    return ((value - mean) * lax.rsqrt(spread + norm_eps) * gain + bias).astype(jnp.bfloat16)


def place_weights(place, ups, downs, up, down, sems):
    z, y, c = place[0], place[1], place[2]

    def start_up():
        for side in range(2):
            core = c ^ side
            for i in range(Z):
                pltpu.make_async_copy(
                    ups[side * Z + i], up.at[z_at(z, core, i), :, core], sems.at[0]
                ).start()

    def start_down():
        for side in range(2):
            core = c ^ side
            for j in range(Y):
                pltpu.make_async_copy(
                    downs[side * Y + j],
                    down.at[:, y_at(y, core, j), core],
                    sems.at[1],
                ).start()

    return start_up, start_down


def ffn_rows(xs, outs, up, down, act, ready_up, ready_down):
    step = 512
    width = up.shape[-1]
    x = jnp.concatenate([r[...] for r in xs], axis=0) if len(xs) > 1 else xs[0][...]
    ready_up()

    def raise_(n, carry):
        cols = pl.ds(pl.multiple_of(n * step, step), step)
        w = up[:, :, :, :, cols].reshape(-1, step)
        upward = jnp.dot(x, w, preferred_element_type=jnp.float32)
        act[:, cols] = jnp.square(jnp.maximum(upward, 0.0)).astype(jnp.bfloat16)
        return carry

    lax.fori_loop(0, width // step, raise_, 0)
    ready_down()
    a = act[...]
    z_step = step // (down.shape[1] * down.shape[2] * down.shape[3])

    def lower(n, carry):
        w = down[pl.ds(n * z_step, z_step)].reshape(step, width)
        part = lax.dot_general(
            a, w, (((1,), (1,)), ((), ())), preferred_element_type=jnp.float32
        ).astype(jnp.bfloat16)
        cols = pl.ds(pl.multiple_of(n * step, step), step)
        at = 0
        for out in outs:
            out[:, cols] = part[at : at + out.shape[0]]
            at += out.shape[0]
        return carry

    lax.fori_loop(0, down.shape[0] // z_step, lower, 0)


def ffn_body(place, *refs, n_in, n_up, n_down):
    xs, refs = refs[:n_in], refs[n_in:]
    ups, downs, refs = refs[:n_up], refs[n_up : n_up + n_down], refs[n_up + n_down :]
    outs, (up, down, act, sems) = refs[:n_in], refs[n_in:]
    start_up, start_down = place_weights(place, ups, downs, up, down, sems)

    def ready_up():
        pltpu.make_async_copy(up, up, sems.at[0]).wait()
        start_down()

    def ready_down():
        pltpu.make_async_copy(down, down, sems.at[1]).wait()

    start_up()
    ffn_rows(xs, outs, up, down, act, ready_up, ready_down)


def ffn(place, xs, ups, downs, hidden):
    rows = sum(x.shape[0] for x in xs)
    width = xs[0].shape[1]
    out = [jax.ShapeDtypeStruct(x.shape, jnp.bfloat16) for x in xs]
    weights = pltpu.VMEM((Z, Y, 2, width // (Z * Y * 2), hidden), jnp.bfloat16)
    return call(
        functools.partial(ffn_body, n_in=len(xs), n_up=len(ups), n_down=len(downs)),
        out,
        (place, *xs, *ups, *downs),
        [SMEM] + [VMEM] * len(xs) + [HBM] * (len(ups) + len(downs)),
        4 * rows * width * hidden,
        28,
        [weights, weights, pltpu.VMEM((rows, hidden), jnp.bfloat16), pltpu.SemaphoreType.DMA((2,))],
    )


def add(a, b):
    return (a.astype(jnp.float32) + b.astype(jnp.float32)).astype(jnp.bfloat16)


def on_device(
    queries, keys, values, residual, sinks, out_weight, up_weight, down_weight, gains, biases
):
    tokens = queries.shape[0]
    rows = residual.shape[0] // 2
    hidden = up_weight.shape[1]
    rank = lax.axis_index("tp")
    s = lax.axis_index("sp")
    place = jnp.stack([s // (2 * Y), s // 2 % Y, s % 2])

    tails = jnp.stack([keys[tokens - WINDOW :], values[tokens - WINDOW :]])
    halo = from_behind(tails, "sp", 1)
    ups = gathered_up(place, up_weight)
    downs = gathered_down(place, down_weight.T)

    info = jnp.stack([rank, s * tokens, s % 2])
    far, first, second, own = attend(info, sinks, queries, keys, values, halo, out_weight, rows)
    from_far = x_first(far)
    from_first = x_first(first)
    from_second = x_second(add(second, from_far))
    normed = norm(residual, gains[0], biases[0], own, from_first, from_second)
    first = x_first(normed)
    second = x_second(normed)
    far = x_first(second)
    weights = (ups, downs, hidden)
    far, first = ffn(place, (far, first), *weights)
    from_far = x_first(far)
    from_first = x_first(first)
    second, own = ffn(place, (second, normed), *weights)
    from_second = x_second(add(second, from_far))
    return norm(normed, gains[1], biases[1], own, from_first, from_second)


def solution(mesh):
    return jax.shard_map(
        on_device,
        mesh=mesh,
        in_specs=(
            P("sp", "tp"),
            P("sp", "tp"),
            P("sp", "tp"),
            P(("sp", "tp"), None),
            P("tp"),
            P("tp", None),
            P("sp", "tp"),
            P("tp", "sp"),
            P(),
            P(),
        ),
        out_specs=P(("sp", "tp"), None),
        check_vma=False,
    )
```
